32 devices in a mesh: ep: 8 (over z, y), tp: 4 (over x, core).
Axes of the slice: x: 2, y: 2, z: 4, core: 2. Of those that a mesh axis runs over, the one named last changes fastest.
Arguments:
- tokens: bfloat16 [24, 2048], P('ep'), may hold values from -6 to 6
- mixer_gain: float32 [2048], replicated, may hold values from 0.1 to 1.9
- query_weight: bfloat16 [2048, 2048], P('ep', 'tp'), may hold values from -0.125 to 0.125
- key_cache: bfloat16 [24, 1024, 4, 128], P('ep', None, 'tp'), may hold values from -6 to 6
- value_cache: bfloat16 [24, 1024, 4, 128], P('ep', None, 'tp'), may hold values from -6 to 6
- seq_lengths: int32 [24], P('ep'), may hold values from 1 to 1024, as said below
- head_offset: float32 [16], P('tp'), may hold values from -8.5 to -3.5
- output_weight: bfloat16 [2048, 2048], P('tp', 'ep'), may hold values from -0.5 to 0.5
- expert_gain: float32 [2048], replicated, may hold values from 0.1 to 1.9
- expert_ids: int32 [24, 2], P('ep'), may hold values from 0 to 7, as said below
- route_weight: float32 [24, 2], P('ep'), may hold values from 0.2 to 1
- gate_weight: bfloat16 [8, 2048, 1024], P('ep', None, 'tp'), may hold values from -0.125 to 0.125
- up_weight: bfloat16 [8, 2048, 1024], P('ep', None, 'tp'), may hold values from -0.125 to 0.125
- down_weight: bfloat16 [8, 1024, 2048], P('ep', 'tp'), may hold values from -0.1875 to 0.1875
Outputs:
- layer_out: bfloat16 [24, 2048], P('ep', 'tp')
The draws below stay inside these ranges and needn't reach their ends.
Inputs may be any that keep to these rules, and one draw needn't show every extreme that they name: `seq_lengths`: some sequence holds all 1024 positions. `expert_ids`: the 2 experts of a row are different and lie in one group of 4 consecutive expert numbers. Among the 3 rows of one index of ep no expert is named by more than 2 rows, and some expert by exactly 2.
All inputs are finite; a program needn't handle non-finite values.
Results may differ from the reference program's by a relative error of at most 0.012.
Values may be sent and summed in bfloat16 or wider, within the bound.
A program may use at most 64 MiB of HBM per device.

```python
import jax
import jax.numpy as jnp
from jax import lax

D = 2048
HEADS = 16
KV_HEADS = 4
HD = 128
FF_E = 1024
EPG = 4
TOP = 2
CACHE = 1024
B_DEV = 3
B_TOT = 24
EXPERTS = 8
GROUPS = 2
CAP = 2
N_TP = 4


def draw_seq_lengths(key, part):
    first = jax.random.randint(jax.random.fold_in(key, 11), (B_TOT,), 1, CACHE + 1)
    second = jax.random.randint(jax.random.fold_in(key, 12), (B_TOT,), 1, CACHE + 1)
    chosen = jax.random.randint(jax.random.fold_in(key, 13), (), 0, B_TOT)
    lengths = jnp.minimum(first, second)
    lengths = jnp.where(jnp.arange(B_TOT) == chosen, CACHE, lengths)
    return lengths.astype(jnp.int32)


def draw_expert_ids(key, part):
    blocks = B_TOT // B_DEV
    group_keys = jax.random.split(jax.random.fold_in(key, 21), blocks)
    group_order = jax.vmap(lambda single: jax.random.permutation(single, GROUPS))(group_keys)
    sets = jnp.arange(B_DEV) // CAP
    groups = group_order[:, sets]
    leads = jax.random.randint(jax.random.fold_in(key, 22), (blocks, GROUPS), 0, EPG)[:, sets]
    other_keys = jax.random.split(jax.random.fold_in(key, 23), blocks * B_DEV)
    others = jax.vmap(lambda single: jax.random.permutation(single, EPG - 1))(other_keys)[:, :TOP - 1] + 1
    others = others.reshape(blocks, B_DEV, TOP - 1)
    inside = jnp.concatenate([leads[:, :, None], (leads[:, :, None] + others) % EPG], axis=2)
    numbers = groups[:, :, None] * EPG + inside
    return numbers.reshape(B_TOT, TOP).astype(jnp.int32)


def block_scale(rng, extent, cuts, smallest, largest):
    loudness, own = 1.0, jax.random.fold_in(rng, 6)
    for axis_at, shards_of in cuts:
        steps = jnp.exp(jax.random.uniform(jax.random.fold_in(own, axis_at), (shards_of,), jnp.float32, smallest / len(cuts), largest / len(cuts)))
        loudness = loudness * jnp.repeat(steps, extent[axis_at] // shards_of).reshape([-1 if axis == axis_at else 1 for axis in range(len(extent))])
    return loudness


def normal_values(key, shape, deviation, most, shards=(), kind=jnp.bfloat16):
    array = jax.random.normal(key, shape, jnp.float32) * deviation
    if len(shards) > 0:
        array = block_scale(key, shape, shards, -0.22, 0.18) * array
    return jnp.clip(array, min=-most, max=most).astype(kind)


def setup_inputs(seed: int = 0) -> dict:
    seeds = jax.random.split(jax.random.key(seed), 15)
    return {
        "tokens": normal_values(seeds[0], (B_TOT, D), 1.0, 6.0, ((0, 8),)),
        "mixer_gain": jnp.clip(1.0 + 0.18 * jax.random.normal(seeds[1], (D,), jnp.float32), 0.1, 1.9),
        "query_weight": normal_values(seeds[2], (D, HEADS * HD), D ** -0.5, 0.125, ((0, 8), (1, 4))),
        "key_cache": normal_values(seeds[3], (B_TOT, CACHE, KV_HEADS, HD), 1.0, 6.0, ((0, 8), (2, 4))),
        "value_cache": normal_values(seeds[4], (B_TOT, CACHE, KV_HEADS, HD), 1.0, 6.0, ((0, 8), (2, 4))),
        "seq_lengths": draw_seq_lengths(jax.random.fold_in(seeds[14], 71), 0),
        "head_offset": jnp.clip(-8.5 + 5.0 * jax.random.uniform(seeds[6], (HEADS,), jnp.float32) ** block_scale(seeds[6], (HEADS,), ((0, 4),), -0.2, 0.2), -8.5, -3.5),
        "output_weight": normal_values(seeds[7], (HEADS * HD, D), HD ** -0.5, 0.5, ((0, 4), (1, 8))),
        "expert_gain": jnp.clip(1.0 + 0.18 * jax.random.normal(seeds[8], (D,), jnp.float32), 0.1, 1.9),
        "expert_ids": draw_expert_ids(jax.random.fold_in(seeds[14], 71), 0),
        "route_weight": jnp.clip(0.2 + 0.8 * jax.random.uniform(seeds[10], (B_TOT, TOP), jnp.float32) ** block_scale(seeds[10], (B_TOT, TOP), ((0, 8),), -0.2, 0.2), 0.2, 1.0),
        "gate_weight": normal_values(seeds[11], (EXPERTS, D, FF_E), D ** -0.5, 0.125, ((0, 8), (2, 4))),
        "up_weight": normal_values(seeds[12], (EXPERTS, D, FF_E), D ** -0.5, 0.125, ((0, 8), (2, 4))),
        "down_weight": normal_values(seeds[13], (EXPERTS, FF_E, D), FF_E ** -0.5, 0.1875, ((0, 8), (1, 4))),
    }


def rms_norm(values, gain):
    wide = values.astype(jnp.float32)
    scale = lax.rsqrt(lax.optimization_barrier(jnp.mean(wide * wide, axis=-1, keepdims=True)) + 1e-06)
    return (wide * scale * gain).astype(jnp.bfloat16)

def reference(tokens, mixer_gain, query_weight, key_cache, value_cache, seq_lengths, head_offset, output_weight, expert_gain, expert_ids, route_weight, gate_weight, up_weight, down_weight):
    normed = rms_norm(tokens, mixer_gain)
    query = jnp.dot(normed, query_weight, preferred_element_type=jnp.float32).astype(jnp.bfloat16)
    per_group = HEADS // KV_HEADS
    scale = HD ** (-0.5)
    offset = head_offset.reshape(KV_HEADS, per_group, 1)

    def attend(args):
        query_row, keys, values, length = args
        grouped = query_row.reshape(KV_HEADS, per_group, HD).astype(jnp.float32)
        score = jnp.einsum('kgd,skd->kgs', grouped, keys.astype(jnp.float32)) * scale + offset
        valid = (jnp.arange(CACHE, dtype=jnp.int32) < length)[None, None, :]
        log_take = jax.nn.log_sigmoid(score)
        log_pass = jnp.where(valid, jax.nn.log_sigmoid(-score), 0.0)
        later = lax.cumsum(log_pass, axis=2, reverse=True) - log_pass
        weight = jnp.where(valid, jnp.exp(log_take + later), 0.0).astype(jnp.bfloat16)
        result = jnp.einsum('kgs,skd->kgd', weight.astype(jnp.float32), values.astype(jnp.float32))
        return result.reshape(HEADS * HD).astype(jnp.bfloat16)
    mixed = lax.map(attend, (query, key_cache, value_cache, seq_lengths))
    quarter_width = HEADS * HD // N_TP
    total = tokens.astype(jnp.float32)
    for quarter in range(N_TP):
        part = jnp.dot(mixed[:, quarter * quarter_width:(quarter + 1) * quarter_width], output_weight[quarter * quarter_width:(quarter + 1) * quarter_width], preferred_element_type=jnp.float32).astype(jnp.bfloat16)
        total = total + lax.optimization_barrier(part).astype(jnp.float32)
    resid = total.astype(jnp.bfloat16)
    normed2 = rms_norm(resid, expert_gain)
    flat_ids = expert_ids.reshape(-1).astype(jnp.int32)
    row_ids = (jnp.arange(B_TOT * TOP, dtype=jnp.int32) // TOP).astype(jnp.int32)
    unit_width = FF_E // N_TP

    def expert(args):
        number, row_index = args
        row = lax.dynamic_slice_in_dim(normed2, row_index, 1, 0)
        gate = jnp.dot(row, gate_weight[number], preferred_element_type=jnp.float32)
        upward = jnp.dot(row, up_weight[number], preferred_element_type=jnp.float32)
        hidden = (jax.nn.silu(gate) * upward).astype(jnp.bfloat16)
        downs = down_weight[number]
        summed = jnp.zeros((1, D), jnp.float32)
        for quarter in range(N_TP):
            part = jnp.dot(hidden[:, quarter * unit_width:(quarter + 1) * unit_width], downs[quarter * unit_width:(quarter + 1) * unit_width], preferred_element_type=jnp.float32).astype(jnp.bfloat16)
            summed = summed + lax.optimization_barrier(part).astype(jnp.float32)
        return summed.astype(jnp.bfloat16)[0]
    outputs = lax.map(expert, (flat_ids, row_ids))
    weighted = outputs.reshape(B_TOT, TOP, D).astype(jnp.float32) * route_weight[:, :, None]
    return (resid.astype(jnp.float32) + lax.optimization_barrier(jnp.sum(weighted, axis=1))).astype(jnp.bfloat16)
```

```python
import jax
import jax.numpy as jnp
from jax import lax
from jax.experimental import pallas as pl
from jax.experimental.pallas import tpu as pltpu
from jax.sharding import PartitionSpec as P

EPG = 4
TOP = 2
BLK = 256


def rms_norm(values, gain):
    wide = values.astype(jnp.float32)
    scale = lax.rsqrt(jnp.mean(wide * wide, axis=-1, keepdims=True) + 1e-06)
    return (wide * scale * gain).astype(jnp.bfloat16)


def attend_cache(query, key_cache, value_cache, seq_lengths, head_offset):
    batch = query.shape[0]
    local_heads = head_offset.shape[0]
    kv_local = key_cache.shape[2]
    head_size = key_cache.shape[3]
    per_group = local_heads // kv_local
    grouped = query.reshape(batch, kv_local, per_group, head_size)
    offset = head_offset.reshape(1, kv_local, per_group, 1)
    scale = head_size ** (-0.5)
    longest = jnp.max(seq_lengths)
    block_count = (longest + BLK - 1) // BLK

    def step(turn, carry):
        total, later = carry
        start = (block_count - 1 - turn) * BLK
        keys = lax.dynamic_slice_in_dim(key_cache, start, BLK, 1)
        values = lax.dynamic_slice_in_dim(value_cache, start, BLK, 1)
        score = (
            jnp.einsum("bkgd,bskd->bkgs", grouped, keys, preferred_element_type=jnp.float32) * scale
            + offset
        )
        places = start + jnp.arange(BLK, dtype=jnp.int32)
        valid = (places[None, :] < seq_lengths[:, None])[:, None, None, :]
        log_take = jax.nn.log_sigmoid(score)
        log_pass = jnp.where(valid, jax.nn.log_sigmoid(-score), 0.0)
        inside = lax.cumsum(log_pass, axis=3, reverse=True) - log_pass + later[..., None]
        weight = jnp.where(valid, jnp.exp(log_take + inside), 0.0).astype(jnp.bfloat16)
        total = total + jnp.einsum(
            "bkgs,bskd->bkgd", weight, values, preferred_element_type=jnp.float32
        )
        return (total, later + jnp.sum(log_pass, axis=3))

    start_total = jnp.zeros((batch, kv_local, per_group, head_size), jnp.float32)
    start_later = jnp.zeros((batch, kv_local, per_group), jnp.float32)
    total, later = lax.fori_loop(0, block_count, step, (start_total, start_later))
    return total.reshape(batch, local_heads * head_size).astype(jnp.bfloat16)


def expert_hidden(rows, gate_weight, up_weight):
    gate = jnp.dot(rows, gate_weight[0], preferred_element_type=jnp.float32)
    upward = jnp.dot(rows, up_weight[0], preferred_element_type=jnp.float32)
    return (jax.nn.silu(gate) * upward).astype(jnp.bfloat16)


def local_collectives(
    tokens,
    mixer_gain,
    query_weight,
    key_cache,
    value_cache,
    seq_lengths,
    head_offset,
    output_weight,
    expert_gain,
    expert_ids,
    route_weight,
    gate_weight,
    up_weight,
    down_weight,
):
    ep_count = lax.axis_size("ep")
    batch = tokens.shape[0]
    normed = rms_norm(tokens, mixer_gain)
    feature_rows = lax.all_to_all(normed, "ep", split_axis=1, concat_axis=0, tiled=True)
    query = lax.psum_scatter(
        jnp.dot(feature_rows, query_weight, preferred_element_type=jnp.float32),
        "ep",
        scatter_dimension=0,
        tiled=True,
    )
    query = query.astype(jnp.bfloat16)
    mixed = attend_cache(query, key_cache, value_cache, seq_lengths, head_offset)
    partial_value = jnp.dot(
        lax.all_gather(mixed, "ep", axis=0, tiled=True),
        output_weight,
        preferred_element_type=jnp.float32,
    ).astype(jnp.bfloat16)
    summed = lax.psum(partial_value, "tp").astype(jnp.float32)
    attention = lax.all_to_all(summed, "ep", split_axis=0, concat_axis=1, tiled=True)
    resid = (tokens.astype(jnp.float32) + attention).astype(jnp.bfloat16)
    normed2 = rms_norm(resid, expert_gain)
    group_total = ep_count // EPG
    slot_count = max(2, (batch + group_total - 1) // group_total)
    pair_count = batch * TOP
    pair_ids = expert_ids.reshape(pair_count)
    order = jnp.arange(pair_count, dtype=jnp.int32)
    earlier = (order[None, :] < order[:, None]) & (pair_ids[:, None] == pair_ids[None, :])
    slot_index = jnp.sum(earlier.astype(jnp.int32), axis=1)
    dest_slot = pair_ids * slot_count + slot_index
    places = jnp.arange(ep_count * slot_count, dtype=jnp.int32)
    dispatch = (places[:, None] == dest_slot[None, :]).astype(jnp.bfloat16)
    pair_rows = jnp.repeat(normed2, TOP, axis=0)
    outgoing = jnp.dot(dispatch, pair_rows, preferred_element_type=jnp.float32).astype(jnp.bfloat16)
    outgoing = outgoing.reshape(ep_count, slot_count, normed2.shape[1])
    received = lax.all_to_all(outgoing, "ep", split_axis=0, concat_axis=0, tiled=True)
    count = received.shape[1]
    flat_rows = received.reshape(ep_count * count, received.shape[2])
    hidden = expert_hidden(flat_rows, gate_weight, up_weight)
    term = jnp.dot(hidden, down_weight[0], preferred_element_type=jnp.float32)
    reduced = lax.psum_scatter(term.astype(jnp.bfloat16), "tp", scatter_dimension=1, tiled=True)
    results = reduced.reshape(ep_count, count, reduced.shape[1])
    returned = lax.all_to_all(results, "ep", split_axis=0, concat_axis=0, tiled=True)
    columns = returned.shape[2]
    picked = jnp.dot(
        dispatch.T,
        returned.reshape(ep_count * slot_count, columns),
        preferred_element_type=jnp.float32,
    )
    weighted = picked.reshape(batch, TOP, columns) * route_weight[:, :, None]
    mixture = jnp.sum(weighted, axis=1)
    slice_width = mixture.shape[1]
    column_start = lax.axis_index("tp") * slice_width
    resid_slice = lax.dynamic_slice_in_dim(resid, column_start, slice_width, 1)
    return (resid_slice.astype(jnp.float32) + mixture).astype(jnp.bfloat16)


MESH = pl.DeviceIdType.MESH
LANES = 128
SUBLANES = 8


def wait_bytes(ref, count, sem):
    view = ref.at[pl.ds(0, count)]
    pltpu.make_async_copy(view, view, sem).wait()


def layer_kernel(
    ep,
    tp,
    tokens_ref,
    mixer_gain_ref,
    expert_gain_ref,
    lengths_ref,
    offset_ref,
    ids_ref,
    route_ref,
    query_hbm,
    key_hbm,
    value_hbm,
    output_hbm,
    gate_hbm,
    up_hbm,
    down_hbm,
    out_ref,
    query_w,
    key_w,
    value_w,
    output_w,
    gate_w,
    up_w,
    down_w,
    load_sem,
    send_sem,
    recv_sem,
    a_send,
    a_recv,
    b_send,
    b_recv,
    c_send,
    c_recv,
    d_send,
    d_recv,
    e_send,
    e_recv,
    f_send,
    f_recv,
    rows_s,
    token_s,
    part_s,
    query_s,
    mixed_s,
    mixed_rows_s,
    resid_s,
    term_s,
):
    me, mt = lax.axis_index("ep"), lax.axis_index("tp")
    total = ep * tp
    flat = me * tp + mt
    batch, width = tokens_ref.shape
    cols = query_w.shape[0]
    heads = offset_ref.shape[0]
    head_size = mixed_s.shape[1] // heads
    cache = key_w.shape[1]
    kv_local = key_w.shape[2] // head_size
    per_group = heads // kv_local
    out_cols = out_ref.shape[1]
    f32, bf16 = jnp.float32, jnp.bfloat16

    loads = []
    for place, (source, target) in enumerate(
        (
            (query_hbm, query_w),
            (key_hbm, key_w),
            (value_hbm, value_w),
            (output_hbm, output_w),
            (gate_hbm, gate_w),
            (up_hbm, up_w),
            (down_hbm, down_w),
        )
    ):
        loads.append(pltpu.make_async_copy(source, target, load_sem.at[place]))
        loads[-1].start()

    barrier = pltpu.get_barrier_semaphore()
    for step in range(1, total):
        other = lax.rem(flat + step, total)
        pl.semaphore_signal(
            barrier, inc=1, device_id=(other // tp, lax.rem(other, tp)), device_id_type=MESH
        )

    def send(phase, source, target, device):
        pltpu.make_async_remote_copy(
            src_ref=source,
            dst_ref=target,
            send_sem=send_sem.at[phase],
            recv_sem=recv_sem.at[phase],
            device_id=device,
            device_id_type=MESH,
        ).start()

    def ep_peers():
        return [lax.rem(me + step, ep) for step in range(1, ep)]

    wide = tokens_ref[...].astype(f32)
    scale = lax.rsqrt(jnp.mean(wide * wide, axis=-1, keepdims=True) + 1e-06)
    normed = wide * scale * mixer_gain_ref[...]
    for e in range(ep):
        a_send[e, 0] = normed[:, e * cols : (e + 1) * cols].astype(bf16)
        a_send[e, 1] = tokens_ref[:, e * cols : (e + 1) * cols]
    query_s[...] = jnp.zeros_like(query_s)
    pl.semaphore_wait(barrier, total - 1)
    for peer in ep_peers():
        send(0, a_send.at[peer], a_recv.at[me], (peer, mt))
    a_recv[me] = a_send[me]

    earlier = lax.broadcasted_iota(jnp.int32, (LANES, 2 * LANES), 0)
    later = lax.broadcasted_iota(jnp.int32, (LANES, 2 * LANES), 1)
    suffix = ((earlier > later) | (later >= LANES)).astype(f32).astype(bf16)
    suffix = jnp.concatenate([suffix] * 3, axis=0)

    loads[0].wait()
    wait_bytes(a_recv, ep - 1, recv_sem.at[0])
    for e in range(ep):
        rows_s[batch * e : batch * (e + 1), :] = a_recv[e, 0].astype(f32)
        token_s[batch * e : batch * (e + 1), :] = a_recv[e, 1].astype(f32)
    part_s[...] = jnp.dot(rows_s[...].astype(bf16), query_w[...], preferred_element_type=f32)
    for e in range(ep):
        b_send[e] = part_s[batch * e : batch * (e + 1), :]
    for peer in ep_peers():
        send(1, b_send.at[peer], b_recv.at[me], (peer, mt))
    b_recv[me] = b_send[me]
    loads[1].wait()
    loads[2].wait()
    wait_bytes(b_recv, ep - 1, recv_sem.at[1])
    query = b_recv[0]
    for e in range(1, ep):
        query = query + b_recv[e]
    query = query.astype(bf16).astype(f32)

    groups = [(row, kv) for row in range(batch) for kv in range(kv_local)]
    places = lax.broadcasted_iota(jnp.int32, (SUBLANES, cache), 1)
    line = lax.broadcasted_iota(jnp.int32, (SUBLANES, 1), 0)
    blocks = cache // LANES
    takes, passes, valids = [], [], []
    for row, kv in groups:
        offset = jnp.zeros((SUBLANES, 1), f32)
        for h in range(per_group):
            head = kv * per_group + h
            query_s[row, kv, h : h + 1, :] = query[
                row : row + 1, head * head_size : (head + 1) * head_size
            ]
            offset = jnp.where(line == h, offset_ref[head], offset)
        keys = key_w[row, :, kv * head_size : (kv + 1) * head_size]
        score = lax.dot_general(
            query_s[row, kv].astype(bf16),
            keys,
            (((1,), (1,)), ((), ())),
            preferred_element_type=f32,
        )
        score = score * (head_size ** (-0.5)) + offset
        valid = places < lengths_ref[row]
        soft = jnp.log1p(jnp.exp(-jnp.abs(score)))
        takes.append(jnp.minimum(score, 0.0) - soft)
        passes.append(jnp.where(valid, jnp.minimum(-score, 0.0) - soft, 0.0))
        valids.append(valid)
    tall = jnp.concatenate(
        [p[:, j * LANES : (j + 1) * LANES] for p in passes for j in range(blocks)], axis=0
    )
    high = tall.astype(bf16)
    rest = tall - high.astype(f32)
    middle = rest.astype(bf16)
    low = (rest - middle.astype(f32)).astype(bf16)
    sums = jnp.dot(
        jnp.concatenate([high, middle, low], axis=1), suffix, preferred_element_type=f32
    )
    for at, (row, kv) in enumerate(groups):
        carry = jnp.zeros((SUBLANES, LANES), f32)
        inside = [None] * blocks
        for j in reversed(range(blocks)):
            top = (at * blocks + j) * SUBLANES
            inside[j] = sums[top : top + SUBLANES, :LANES] + carry
            carry = carry + sums[top : top + SUBLANES, LANES:]
        weight = jnp.where(
            valids[at], jnp.exp(takes[at] + jnp.concatenate(inside, axis=1)), 0.0
        ).astype(bf16)
        values = value_w[row, :, kv * head_size : (kv + 1) * head_size]
        mixed = jnp.dot(weight, values, preferred_element_type=f32)
        for h in range(per_group):
            head = kv * per_group + h
            mixed_s[row : row + 1, head * head_size : (head + 1) * head_size] = mixed[h : h + 1, :]
    c_send[...] = mixed_s[...].astype(bf16)
    for peer in ep_peers():
        send(2, c_send, c_recv.at[me], (peer, mt))
    c_recv[me] = c_send[...]
    loads[3].wait()
    wait_bytes(c_recv, ep - 1, recv_sem.at[2])
    for e in range(ep):
        mixed_rows_s[batch * e : batch * (e + 1), :] = c_recv[e].astype(f32)

    d_send[...] = jnp.dot(
        mixed_rows_s[...].astype(bf16), output_w[...], preferred_element_type=f32
    ).astype(bf16)
    for step in range(1, tp):
        send(3, d_send, d_recv.at[mt], (me, lax.rem(mt + step, tp)))
    d_recv[mt] = d_send[...]
    wait_bytes(d_recv, tp - 1, recv_sem.at[3])
    resid = token_s[...]
    for t in range(tp):
        resid = resid + d_recv[t].astype(f32)
    e_send[...] = resid.astype(bf16)

    for peer in ep_peers():
        send(4, e_send, e_recv.at[me], (peer, mt))
    e_recv[me] = e_send[...]
    numbers = ids_ref[...]
    routes = route_ref[...]
    shares = [
        jnp.sum(jnp.where(numbers == e, routes, 0.0), axis=1, keepdims=True) for e in range(ep)
    ]
    loads[4].wait()
    loads[5].wait()
    loads[6].wait()
    wait_bytes(e_recv, ep - 1, recv_sem.at[4])
    square = None
    for e in range(ep):
        block = e_recv[e].astype(f32)
        resid_s[e] = block
        square = block * block if square is None else square + block * block
    scale = lax.rsqrt(jnp.sum(square, axis=-1, keepdims=True) / width + 1e-06)
    normed2 = jnp.concatenate(
        [
            (resid_s[e] * scale * expert_gain_ref[:, e * cols : (e + 1) * cols]).astype(bf16)
            for e in range(ep)
        ],
        axis=1,
    )
    gate = jnp.dot(normed2, gate_w[0], preferred_element_type=f32)
    upward = jnp.dot(normed2, up_w[0], preferred_element_type=f32)
    hidden = (gate / (1.0 + jnp.exp(-gate)) * upward).astype(bf16)
    term_s[...] = jnp.dot(hidden, down_w[0], preferred_element_type=f32)
    for e in range(ep):
        for t in range(tp):
            f_send[e * tp + t] = term_s[
                batch * e : batch * (e + 1), t * out_cols : (t + 1) * out_cols
            ].astype(bf16)
    for step in range(1, total):
        other = lax.rem(flat + step, total)
        send(5, f_send.at[other], f_recv.at[flat], (other // tp, lax.rem(other, tp)))
    f_recv[flat] = f_send[flat]
    own_blocks = out_cols // cols
    row_at = lax.broadcasted_iota(jnp.int32, (batch, ep * batch), 0) + me * batch
    column_at = lax.broadcasted_iota(jnp.int32, (batch, ep * batch), 1)
    own_rows = (row_at == column_at).astype(f32).astype(bf16)
    own_resid = jnp.concatenate(
        [e_recv[mt * own_blocks + j] for j in range(own_blocks)], axis=1
    )
    result = jnp.dot(own_rows, own_resid, preferred_element_type=f32)
    wait_bytes(f_recv, total - 1, recv_sem.at[5])
    mixture = jnp.zeros_like(result)
    for e in range(ep):
        summed = f_recv[e * tp].astype(f32)
        for t in range(1, tp):
            summed = summed + f_recv[e * tp + t].astype(f32)
        mixture = mixture + summed.astype(bf16).astype(f32) * shares[e]
    out_ref[...] = (result + mixture).astype(bf16)

    wait_bytes(a_recv, ep - 1, send_sem.at[0])
    wait_bytes(b_recv, ep - 1, send_sem.at[1])
    wait_bytes(c_recv, ep - 1, send_sem.at[2])
    wait_bytes(d_recv, tp - 1, send_sem.at[3])
    wait_bytes(e_recv, ep - 1, send_sem.at[4])
    wait_bytes(f_recv, total - 1, send_sem.at[5])


def local_kernel(
    tokens,
    mixer_gain,
    query_weight,
    key_cache,
    value_cache,
    seq_lengths,
    head_offset,
    output_weight,
    expert_gain,
    expert_ids,
    route_weight,
    gate_weight,
    up_weight,
    down_weight,
):
    ep, tp = lax.axis_size("ep"), lax.axis_size("tp")
    batch, width = tokens.shape
    cols, heads_width = query_weight.shape
    out_cols = width // tp
    rows = ep * batch
    heads = head_offset.shape[0]
    cache, kv_local, head_size = key_cache.shape[1:]
    keys = key_cache.reshape(batch, cache, kv_local * head_size)
    values = value_cache.reshape(batch, cache, kv_local * head_size)
    big = (query_weight, keys, values, output_weight, gate_weight, up_weight, down_weight)
    f32, bf16 = jnp.float32, jnp.bfloat16
    vmem = pl.BlockSpec(memory_space=pltpu.VMEM)
    smem = pl.BlockSpec(memory_space=pltpu.SMEM)
    hbm = pl.BlockSpec(memory_space=pl.ANY)

    def body(*refs):
        layer_kernel(ep, tp, *refs)

    return pl.pallas_call(
        body,
        out_shape=jax.ShapeDtypeStruct((batch, out_cols), bf16),
        in_specs=[vmem, vmem, vmem, smem, smem, vmem, vmem] + [hbm] * len(big),
        out_specs=vmem,
        scratch_shapes=[pltpu.VMEM(array.shape, array.dtype) for array in big]
        + [
            pltpu.SemaphoreType.DMA((len(big),)),
            pltpu.SemaphoreType.DMA((6,)),
            pltpu.SemaphoreType.DMA((6,)),
            pltpu.VMEM((ep, 2, batch, cols), bf16),
            pltpu.VMEM((ep, 2, batch, cols), bf16),
            pltpu.VMEM((ep, batch, heads_width), f32),
            pltpu.VMEM((ep, batch, heads_width), f32),
            pltpu.VMEM((batch, heads_width), bf16),
            pltpu.VMEM((ep, batch, heads_width), bf16),
            pltpu.VMEM((rows, cols), bf16),
            pltpu.VMEM((tp, rows, cols), bf16),
            pltpu.VMEM((rows, cols), bf16),
            pltpu.VMEM((ep, rows, cols), bf16),
            pltpu.VMEM((ep * tp, batch, out_cols), bf16),
            pltpu.VMEM((ep * tp, batch, out_cols), bf16),
            pltpu.VMEM((rows, cols), f32),
            pltpu.VMEM((rows, cols), f32),
            pltpu.VMEM((rows, heads_width), f32),
            pltpu.VMEM((batch, kv_local, SUBLANES, head_size), f32),
            pltpu.VMEM((batch, heads_width), f32),
            pltpu.VMEM((rows, heads_width), f32),
            pltpu.VMEM((ep, rows, cols), f32),
            pltpu.VMEM((rows, width), f32),
        ],
        compiler_params=pltpu.CompilerParams(
            collective_id=0, has_side_effects=True, vmem_limit_bytes=60 * 1024 * 1024
        ),
    )(
        tokens,
        mixer_gain.reshape(1, width),
        expert_gain.reshape(1, width),
        seq_lengths,
        head_offset,
        expert_ids,
        route_weight,
        *big,
    )


def local(*arrays):
    tokens, query_weight = arrays[0], arrays[2]
    key_cache, head_offset = arrays[3], arrays[6]
    cols = query_weight.shape[0]
    out_cols = tokens.shape[1] // lax.axis_size("tp")
    cache, kv_local, head_size = key_cache.shape[1:]
    whole_tiles = cols % LANES == 0 and head_size % LANES == 0 and cache % LANES == 0
    if whole_tiles and out_cols % cols == 0 and head_offset.shape[0] // kv_local <= SUBLANES:
        return local_kernel(*arrays)
    return local_collectives(*arrays)


def solution(mesh):
    in_specs = (
        P("ep", None),
        P(),
        P("ep", "tp"),
        P("ep", None, "tp", None),
        P("ep", None, "tp", None),
        P("ep"),
        P("tp"),
        P("tp", "ep"),
        P(),
        P("ep", None),
        P("ep", None),
        P("ep", None, "tp"),
        P("ep", None, "tp"),
        P("ep", "tp", None),
    )
    out_specs = P("ep", "tp")
    return jax.shard_map(local, mesh=mesh, in_specs=in_specs, out_specs=out_specs, check_vma=False)
```

```python
import jax
import jax.numpy as jnp
from jax import lax
from jax.experimental import pallas as pl
from jax.experimental.pallas import tpu as pltpu
from jax.sharding import PartitionSpec as P

EPG = 4
TOP = 2
BLK = 256


def rms_norm(values, gain):
    wide = values.astype(jnp.float32)
    scale = lax.rsqrt(jnp.mean(wide * wide, axis=-1, keepdims=True) + 1e-06)
    return (wide * scale * gain).astype(jnp.bfloat16)


def attend_cache(query, key_cache, value_cache, seq_lengths, head_offset):
    batch = query.shape[0]
    local_heads = head_offset.shape[0]
    kv_local = key_cache.shape[2]
    head_size = key_cache.shape[3]
    per_group = local_heads // kv_local
    grouped = query.reshape(batch, kv_local, per_group, head_size)
    offset = head_offset.reshape(1, kv_local, per_group, 1)
    scale = head_size ** (-0.5)
    longest = jnp.max(seq_lengths)
    block_count = (longest + BLK - 1) // BLK

    def step(turn, carry):
        total, later = carry
        start = (block_count - 1 - turn) * BLK
        keys = lax.dynamic_slice_in_dim(key_cache, start, BLK, 1)
        values = lax.dynamic_slice_in_dim(value_cache, start, BLK, 1)
        score = (
            jnp.einsum("bkgd,bskd->bkgs", grouped, keys, preferred_element_type=jnp.float32) * scale
            + offset
        )
        places = start + jnp.arange(BLK, dtype=jnp.int32)
        valid = (places[None, :] < seq_lengths[:, None])[:, None, None, :]
        log_take = jax.nn.log_sigmoid(score)
        log_pass = jnp.where(valid, jax.nn.log_sigmoid(-score), 0.0)
        inside = lax.cumsum(log_pass, axis=3, reverse=True) - log_pass + later[..., None]
        weight = jnp.where(valid, jnp.exp(log_take + inside), 0.0).astype(jnp.bfloat16)
        total = total + jnp.einsum(
            "bkgs,bskd->bkgd", weight, values, preferred_element_type=jnp.float32
        )
        return (total, later + jnp.sum(log_pass, axis=3))

    start_total = jnp.zeros((batch, kv_local, per_group, head_size), jnp.float32)
    start_later = jnp.zeros((batch, kv_local, per_group), jnp.float32)
    total, later = lax.fori_loop(0, block_count, step, (start_total, start_later))
    return total.reshape(batch, local_heads * head_size).astype(jnp.bfloat16)


def expert_hidden(rows, gate_weight, up_weight):
    gate = jnp.dot(rows, gate_weight[0], preferred_element_type=jnp.float32)
    upward = jnp.dot(rows, up_weight[0], preferred_element_type=jnp.float32)
    return (jax.nn.silu(gate) * upward).astype(jnp.bfloat16)


def local_collectives(
    tokens,
    mixer_gain,
    query_weight,
    key_cache,
    value_cache,
    seq_lengths,
    head_offset,
    output_weight,
    expert_gain,
    expert_ids,
    route_weight,
    gate_weight,
    up_weight,
    down_weight,
):
    ep_count = lax.axis_size("ep")
    batch = tokens.shape[0]
    normed = rms_norm(tokens, mixer_gain)
    feature_rows = lax.all_to_all(normed, "ep", split_axis=1, concat_axis=0, tiled=True)
    query = lax.psum_scatter(
        jnp.dot(feature_rows, query_weight, preferred_element_type=jnp.float32),
        "ep",
        scatter_dimension=0,
        tiled=True,
    )
    query = query.astype(jnp.bfloat16)
    mixed = attend_cache(query, key_cache, value_cache, seq_lengths, head_offset)
    partial_value = jnp.dot(
        lax.all_gather(mixed, "ep", axis=0, tiled=True),
        output_weight,
        preferred_element_type=jnp.float32,
    ).astype(jnp.bfloat16)
    summed = lax.psum(partial_value, "tp").astype(jnp.float32)
    attention = lax.all_to_all(summed, "ep", split_axis=0, concat_axis=1, tiled=True)
    resid = (tokens.astype(jnp.float32) + attention).astype(jnp.bfloat16)
    normed2 = rms_norm(resid, expert_gain)
    group_total = ep_count // EPG
    slot_count = max(2, (batch + group_total - 1) // group_total)
    pair_count = batch * TOP
    pair_ids = expert_ids.reshape(pair_count)
    order = jnp.arange(pair_count, dtype=jnp.int32)
    earlier = (order[None, :] < order[:, None]) & (pair_ids[:, None] == pair_ids[None, :])
    slot_index = jnp.sum(earlier.astype(jnp.int32), axis=1)
    dest_slot = pair_ids * slot_count + slot_index
    places = jnp.arange(ep_count * slot_count, dtype=jnp.int32)
    dispatch = (places[:, None] == dest_slot[None, :]).astype(jnp.bfloat16)
    pair_rows = jnp.repeat(normed2, TOP, axis=0)
    outgoing = jnp.dot(dispatch, pair_rows, preferred_element_type=jnp.float32).astype(jnp.bfloat16)
    outgoing = outgoing.reshape(ep_count, slot_count, normed2.shape[1])
    received = lax.all_to_all(outgoing, "ep", split_axis=0, concat_axis=0, tiled=True)
    count = received.shape[1]
    flat_rows = received.reshape(ep_count * count, received.shape[2])
    hidden = expert_hidden(flat_rows, gate_weight, up_weight)
    term = jnp.dot(hidden, down_weight[0], preferred_element_type=jnp.float32)
    reduced = lax.psum_scatter(term.astype(jnp.bfloat16), "tp", scatter_dimension=1, tiled=True)
    results = reduced.reshape(ep_count, count, reduced.shape[1])
    returned = lax.all_to_all(results, "ep", split_axis=0, concat_axis=0, tiled=True)
    columns = returned.shape[2]
    picked = jnp.dot(
        dispatch.T,
        returned.reshape(ep_count * slot_count, columns),
        preferred_element_type=jnp.float32,
    )
    weighted = picked.reshape(batch, TOP, columns) * route_weight[:, :, None]
    mixture = jnp.sum(weighted, axis=1)
    slice_width = mixture.shape[1]
    column_start = lax.axis_index("tp") * slice_width
    resid_slice = lax.dynamic_slice_in_dim(resid, column_start, slice_width, 1)
    return (resid_slice.astype(jnp.float32) + mixture).astype(jnp.bfloat16)


MESH = pl.DeviceIdType.MESH
LANES = 128
SUBLANES = 8


def wait_bytes(ref, count, sem):
    view = ref.at[pl.ds(0, count)]
    pltpu.make_async_copy(view, view, sem).wait()


def layer_kernel(
    ep,
    tp,
    tokens_ref,
    mixer_gain_ref,
    expert_gain_ref,
    lengths_ref,
    offset_ref,
    ids_ref,
    route_ref,
    query_hbm,
    key_hbm,
    value_hbm,
    output_hbm,
    gate_hbm,
    up_hbm,
    down_hbm,
    out_ref,
    query_w,
    key_w,
    value_w,
    output_w,
    gate_w,
    up_w,
    down_w,
    load_sem,
    send_sem,
    recv_sem,
    a_send,
    a_recv,
    b_send,
    b_recv,
    c_send,
    c_recv,
    d_send,
    d_recv,
    e_send,
    e_recv,
    f_send,
    f_recv,
    rows_s,
    token_s,
    part_s,
    query_s,
    mixed_s,
    mixed_rows_s,
    term_s,
    block_sem,
    i_send,
    i_recv,
    answer_s,
):
    me, mt = lax.axis_index("ep"), lax.axis_index("tp")
    total = ep * tp
    flat = me * tp + mt
    batch, width = tokens_ref.shape
    cols = query_w.shape[0]
    heads = offset_ref.shape[0]
    head_size = mixed_s.shape[1] // heads
    cache = key_w.shape[1]
    kv_local = key_w.shape[2] // head_size
    per_group = heads // kv_local
    slots = f_send.shape[1]
    key_tiles = i_send.shape[1] // LANES
    out_cols = out_ref.shape[1]
    f32, bf16 = jnp.float32, jnp.bfloat16

    loads = []
    for place, (source, target) in enumerate(
        (
            (query_hbm, query_w),
            (key_hbm, key_w),
            (value_hbm, value_w),
            (output_hbm, output_w),
            (gate_hbm, gate_w),
            (up_hbm, up_w),
            (down_hbm, down_w),
        )
    ):
        loads.append(pltpu.make_async_copy(source, target, load_sem.at[place]))
        loads[-1].start()

    barrier = pltpu.get_barrier_semaphore()
    greeted = [(lax.rem(me + step, ep), mt) for step in range(1, ep)]
    greeted += [(me, lax.rem(mt + step, tp)) for step in range(1, tp)]
    for device in greeted:
        pl.semaphore_signal(barrier, inc=1, device_id=device, device_id_type=MESH)

    def send(phase, source, target, device):
        pltpu.make_async_remote_copy(
            src_ref=source,
            dst_ref=target,
            send_sem=send_sem.at[phase],
            recv_sem=recv_sem.at[phase],
            device_id=device,
            device_id_type=MESH,
        ).start()

    def ep_peers():
        return [lax.rem(me + step, ep) for step in range(1, ep)]

    wide = tokens_ref[...].astype(f32)
    scale = lax.rsqrt(jnp.mean(wide * wide, axis=-1, keepdims=True) + 1e-06)
    normed = wide * scale * mixer_gain_ref[...]
    for e in range(ep):
        a_send[e, 0] = normed[:, e * cols : (e + 1) * cols].astype(bf16)
        a_send[e, 1] = tokens_ref[:, e * cols : (e + 1) * cols]
    query_s[...] = jnp.zeros_like(query_s)
    keys_own = []
    for row in range(batch):
        for k in range(TOP):
            slot = jnp.int32(0)
            for past in range(row):
                for other in range(TOP):
                    slot += jnp.where(ids_ref[other, past] == ids_ref[k, row], 1, 0)
            keys_own.append(ids_ref[k, row] * slots + slot)
    lane = lax.broadcasted_iota(jnp.int32, (1, LANES * key_tiles), 1)
    for k in range(TOP):
        placed = jnp.zeros(lane.shape, jnp.int32)
        for row in range(batch):
            placed = jnp.where(lane == me * batch + row, keys_own[row * TOP + k], placed)
        i_send[k : k + 1, :] = placed
    pl.semaphore_wait(barrier, len(greeted))
    for peer in ep_peers():
        send(0, a_send.at[peer], a_recv.at[me], (peer, mt))
    a_recv[me] = a_send[me]
    for peer in ep_peers():
        send(6, i_send, i_recv.at[me], (peer, mt))
    i_recv[me] = i_send[...]

    earlier = lax.broadcasted_iota(jnp.int32, (LANES, 2 * LANES), 0)
    later = lax.broadcasted_iota(jnp.int32, (LANES, 2 * LANES), 1)
    suffix = ((earlier > later) | (later >= LANES)).astype(f32).astype(bf16)
    suffix = jnp.concatenate([suffix] * 3, axis=0)

    loads[0].wait()
    wait_bytes(a_recv, ep - 1, recv_sem.at[0])
    for e in range(ep):
        rows_s[batch * e : batch * (e + 1), :] = a_recv[e, 0].astype(f32)
        token_s[batch * e : batch * (e + 1), :] = a_recv[e, 1].astype(f32)
    part_s[...] = jnp.dot(rows_s[...].astype(bf16), query_w[...], preferred_element_type=f32)
    for e in range(ep):
        b_send[e] = part_s[batch * e : batch * (e + 1), :].astype(bf16)
    for peer in ep_peers():
        send(1, b_send.at[peer], b_recv.at[me], (peer, mt))
    b_recv[me] = b_send[me]
    loads[1].wait()
    loads[2].wait()
    wait_bytes(b_recv, ep - 1, recv_sem.at[1])
    query = b_recv[0].astype(f32)
    for e in range(1, ep):
        query = query + b_recv[e].astype(f32)
    query = query.astype(bf16).astype(f32)

    groups = [(row, kv) for row in range(batch) for kv in range(kv_local)]
    places = lax.broadcasted_iota(jnp.int32, (SUBLANES, cache), 1)
    line = lax.broadcasted_iota(jnp.int32, (SUBLANES, 1), 0)
    blocks = cache // LANES
    takes, passes, valids = [], [], []
    for row, kv in groups:
        offset = jnp.zeros((SUBLANES, 1), f32)
        for h in range(per_group):
            head = kv * per_group + h
            query_s[row, kv, h : h + 1, :] = query[
                row : row + 1, head * head_size : (head + 1) * head_size
            ]
            offset = jnp.where(line == h, offset_ref[head], offset)
        keys = key_w[row, :, kv * head_size : (kv + 1) * head_size]
        score = lax.dot_general(
            query_s[row, kv].astype(bf16),
            keys,
            (((1,), (1,)), ((), ())),
            preferred_element_type=f32,
        )
        score = score * (head_size ** (-0.5)) + offset
        valid = places < lengths_ref[row]
        soft = jnp.log1p(jnp.exp(-jnp.abs(score)))
        takes.append(jnp.minimum(score, 0.0) - soft)
        passes.append(jnp.where(valid, jnp.minimum(-score, 0.0) - soft, 0.0))
        valids.append(valid)
    tall = jnp.concatenate(
        [p[:, j * LANES : (j + 1) * LANES] for p in passes for j in range(blocks)], axis=0
    )
    high = tall.astype(bf16)
    rest = tall - high.astype(f32)
    middle = rest.astype(bf16)
    low = (rest - middle.astype(f32)).astype(bf16)
    sums = jnp.dot(
        jnp.concatenate([high, middle, low], axis=1), suffix, preferred_element_type=f32
    )
    for at, (row, kv) in enumerate(groups):
        carry = jnp.zeros((SUBLANES, LANES), f32)
        inside = [None] * blocks
        for j in reversed(range(blocks)):
            top = (at * blocks + j) * SUBLANES
            inside[j] = sums[top : top + SUBLANES, :LANES] + carry
            carry = carry + sums[top : top + SUBLANES, LANES:]
        weight = jnp.where(
            valids[at], jnp.exp(takes[at] + jnp.concatenate(inside, axis=1)), 0.0
        ).astype(bf16)
        values = value_w[row, :, kv * head_size : (kv + 1) * head_size]
        mixed = jnp.dot(weight, values, preferred_element_type=f32)
        for h in range(per_group):
            head = kv * per_group + h
            mixed_s[row : row + 1, head * head_size : (head + 1) * head_size] = mixed[h : h + 1, :]
    c_send[...] = mixed_s[...].astype(bf16)
    for peer in ep_peers():
        send(2, c_send, c_recv.at[me], (peer, mt))
    c_recv[me] = c_send[...]
    loads[3].wait()
    wait_bytes(c_recv, ep - 1, recv_sem.at[2])
    for e in range(ep):
        mixed_rows_s[batch * e : batch * (e + 1), :] = c_recv[e].astype(f32)

    d_send[...] = jnp.dot(
        mixed_rows_s[...].astype(bf16), output_w[...], preferred_element_type=f32
    ).astype(bf16)
    for step in range(1, tp):
        send(3, d_send, d_recv.at[mt], (me, lax.rem(mt + step, tp)))
    d_recv[mt] = d_send[...]
    wait_bytes(d_recv, tp - 1, recv_sem.at[3])
    resid = token_s[...]
    for t in range(tp):
        resid = resid + d_recv[t].astype(f32)
    e_send[...] = resid.astype(bf16)

    for step in range(1, ep):
        pltpu.make_async_remote_copy(
            src_ref=e_send,
            dst_ref=e_recv.at[me],
            send_sem=send_sem.at[4],
            recv_sem=block_sem.at[me],
            device_id=(lax.rem(me + step, ep), mt),
            device_id_type=MESH,
        ).start()
    e_recv[me] = e_send[...]

    wait_bytes(i_recv, ep - 1, recv_sem.at[6])
    keys_all = i_recv[0]
    for e in range(1, ep):
        keys_all = keys_all + i_recv[e]
    rows = ep * batch
    pack_rows = lax.broadcasted_iota(jnp.int32, (ep * slots, rows), 0)
    pack_cols = lax.broadcasted_iota(jnp.int32, (ep * slots, rows), 1)
    row_owner = jnp.zeros_like(pack_rows)
    col_owner = jnp.zeros_like(pack_cols)
    for e in range(1, ep):
        row_owner = row_owner + jnp.where(pack_rows >= e * slots, 1, 0)
        col_owner = col_owner + jnp.where(pack_cols >= e * batch, 1, 0)
    wanted = pack_rows - row_owner * slots + me * slots
    named = wanted == keys_all[0:1, :rows]
    for k in range(1, TOP):
        named = named | (wanted == keys_all[k : k + 1, :rows])
    pack = jnp.where(named & (row_owner == col_owner), 1.0, 0.0).astype(bf16)
    pick_rows = lax.broadcasted_iota(jnp.int32, (batch, ep * slots), 0)
    pick_cols = lax.broadcasted_iota(jnp.int32, (batch, ep * slots), 1)
    line = lax.broadcasted_iota(jnp.int32, (batch, 1), 0)
    picks, routes = [], []
    for k in range(TOP):
        chosen = jnp.zeros_like(pick_rows)
        route = jnp.zeros((batch, 1), f32)
        for row in range(batch):
            chosen = jnp.where(pick_rows == row, keys_own[row * TOP + k], chosen)
            route = jnp.where(line == row, route_ref[k, row], route)
        picks.append(jnp.where(pick_cols == chosen, 1.0, 0.0).astype(bf16))
        routes.append(route)
    row_at = lax.broadcasted_iota(jnp.int32, (batch, rows), 0) + me * batch
    column_at = lax.broadcasted_iota(jnp.int32, (batch, rows), 1)
    own_rows = (row_at == column_at).astype(f32).astype(bf16)

    loads[4].wait()
    loads[5].wait()
    loads[6].wait()
    order = [0]
    for step in range(1, ep // 2 + 1):
        order += [step, ep - step]
    square = gate = upward = None
    for step in list(dict.fromkeys(order))[:ep]:
        source = lax.rem(me + step, ep)
        if step:
            pltpu.make_async_copy(e_send, e_recv.at[source], block_sem.at[source]).wait()
        first = pl.multiple_of(source * cols, cols)
        block = e_recv[source].astype(f32)
        scaled = (block * expert_gain_ref[:, pl.ds(first, cols)]).astype(bf16)
        terms = (
            jnp.sum(block * block, axis=-1, keepdims=True),
            jnp.dot(scaled, gate_w[0, pl.ds(first, cols), :], preferred_element_type=f32),
            jnp.dot(scaled, up_w[0, pl.ds(first, cols), :], preferred_element_type=f32),
        )
        if square is None:
            square, gate, upward = terms
        else:
            square, gate, upward = square + terms[0], gate + terms[1], upward + terms[2]
    scale = lax.rsqrt(square / width + 1e-06)
    gate, upward = gate * scale, upward * scale
    hidden = (gate / (1.0 + jnp.exp(-gate)) * upward).astype(bf16)
    packed = jnp.dot(pack, hidden, preferred_element_type=f32).astype(bf16)
    term_s[...] = jnp.dot(packed, down_w[0], preferred_element_type=f32)
    for e in range(ep):
        for t in range(tp):
            f_send[e * tp + t] = term_s[
                slots * e : slots * (e + 1), t * out_cols : (t + 1) * out_cols
            ].astype(bf16)
    for step in range(1, total):
        other = lax.rem(flat + step, total)
        send(5, f_send.at[other], f_recv.at[flat], (other // tp, lax.rem(other, tp)))
    f_recv[flat] = f_send[flat]
    own_blocks = out_cols // cols
    own_resid = jnp.concatenate(
        [e_recv[mt * own_blocks + j] for j in range(own_blocks)], axis=1
    )
    result = jnp.dot(own_rows, own_resid, preferred_element_type=f32)
    wait_bytes(f_recv, total - 1, recv_sem.at[5])
    for e in range(ep):
        summed = f_recv[e * tp].astype(f32)
        for t in range(1, tp):
            summed = summed + f_recv[e * tp + t].astype(f32)
        answer_s[slots * e : slots * (e + 1), :] = summed
    answers = answer_s[...].astype(bf16)
    mixture = jnp.zeros_like(result)
    for pick, route in zip(picks, routes):
        mixture = mixture + route * jnp.dot(pick, answers, preferred_element_type=f32)
    out_ref[...] = (result + mixture).astype(bf16)

    wait_bytes(a_recv, ep - 1, send_sem.at[0])
    wait_bytes(b_recv, ep - 1, send_sem.at[1])
    wait_bytes(c_recv, ep - 1, send_sem.at[2])
    wait_bytes(d_recv, tp - 1, send_sem.at[3])
    wait_bytes(e_recv, ep - 1, send_sem.at[4])
    wait_bytes(i_recv, ep - 1, send_sem.at[6])
    wait_bytes(f_recv, total - 1, send_sem.at[5])


def local_kernel(
    tokens,
    mixer_gain,
    query_weight,
    key_cache,
    value_cache,
    seq_lengths,
    head_offset,
    output_weight,
    expert_gain,
    expert_ids,
    route_weight,
    gate_weight,
    up_weight,
    down_weight,
):
    ep, tp = lax.axis_size("ep"), lax.axis_size("tp")
    batch, width = tokens.shape
    cols, heads_width = query_weight.shape
    out_cols = width // tp
    rows = ep * batch
    groups = ep // EPG
    slots = max(2, (batch + groups - 1) // groups)
    key_lanes = (rows + LANES - 1) // LANES * LANES
    heads = head_offset.shape[0]
    cache, kv_local, head_size = key_cache.shape[1:]
    keys = key_cache.reshape(batch, cache, kv_local * head_size)
    values = value_cache.reshape(batch, cache, kv_local * head_size)
    big = (query_weight, keys, values, output_weight, gate_weight, up_weight, down_weight)
    f32, bf16 = jnp.float32, jnp.bfloat16
    vmem = pl.BlockSpec(memory_space=pltpu.VMEM)
    smem = pl.BlockSpec(memory_space=pltpu.SMEM)
    hbm = pl.BlockSpec(memory_space=pl.ANY)

    def body(*refs):
        layer_kernel(ep, tp, *refs)

    return pl.pallas_call(
        body,
        out_shape=pltpu.VMEM((batch, out_cols), bf16),
        in_specs=[vmem, vmem, vmem, smem, smem, smem, smem] + [hbm] * len(big),
        out_specs=vmem,
        scratch_shapes=[pltpu.VMEM(array.shape, array.dtype) for array in big]
        + [
            pltpu.SemaphoreType.DMA((len(big),)),
            pltpu.SemaphoreType.DMA((7,)),
            pltpu.SemaphoreType.DMA((7,)),
            pltpu.VMEM((ep, 2, batch, cols), bf16),
            pltpu.VMEM((ep, 2, batch, cols), bf16),
            pltpu.VMEM((ep, batch, heads_width), bf16),
            pltpu.VMEM((ep, batch, heads_width), bf16),
            pltpu.VMEM((batch, heads_width), bf16),
            pltpu.VMEM((ep, batch, heads_width), bf16),
            pltpu.VMEM((rows, cols), bf16),
            pltpu.VMEM((tp, rows, cols), bf16),
            pltpu.VMEM((rows, cols), bf16),
            pltpu.VMEM((ep, rows, cols), bf16),
            pltpu.VMEM((ep * tp, slots, out_cols), bf16),
            pltpu.VMEM((ep * tp, slots, out_cols), bf16),
            pltpu.VMEM((rows, cols), f32),
            pltpu.VMEM((rows, cols), f32),
            pltpu.VMEM((rows, heads_width), f32),
            pltpu.VMEM((batch, kv_local, SUBLANES, head_size), f32),
            pltpu.VMEM((batch, heads_width), f32),
            pltpu.VMEM((rows, heads_width), f32),
            pltpu.VMEM((ep * slots, width), f32),
            pltpu.SemaphoreType.DMA((ep,)),
            pltpu.VMEM((TOP, key_lanes), jnp.int32),
            pltpu.VMEM((ep, TOP, key_lanes), jnp.int32),
            pltpu.VMEM((ep * slots, out_cols), f32),
        ],
        compiler_params=pltpu.CompilerParams(
            collective_id=0, has_side_effects=True, vmem_limit_bytes=60 * 1024 * 1024
        ),
    )(
        tokens,
        mixer_gain.reshape(1, width),
        expert_gain.reshape(1, width),
        seq_lengths,
        head_offset,
        expert_ids.T,
        route_weight.T,
        *big,
    )


def local(*arrays):
    tokens, query_weight = arrays[0], arrays[2]
    key_cache, head_offset = arrays[3], arrays[6]
    cols = query_weight.shape[0]
    out_cols = tokens.shape[1] // lax.axis_size("tp")
    cache, kv_local, head_size = key_cache.shape[1:]
    whole_tiles = cols % LANES == 0 and head_size % LANES == 0 and cache % LANES == 0
    if whole_tiles and out_cols % cols == 0 and head_offset.shape[0] // kv_local <= SUBLANES:
        return local_kernel(*arrays)
    return local_collectives(*arrays)


def solution(mesh):
    in_specs = (
        P("ep", None),
        P(),
        P("ep", "tp"),
        P("ep", None, "tp", None),
        P("ep", None, "tp", None),
        P("ep"),
        P("tp"),
        P("tp", "ep"),
        P(),
        P("ep", None),
        P("ep", None),
        P("ep", None, "tp"),
        P("ep", None, "tp"),
        P("ep", "tp", None),
    )
    out_specs = P("ep", "tp")
    return jax.shard_map(local, mesh=mesh, in_specs=in_specs, out_specs=out_specs, check_vma=False)
```
